32 devices in a mesh: ep: 8 (over z, core), tp: 4 (over y, x).
Axes of the slice: x: 2, y: 2, z: 4, core: 2. Of those that a mesh axis runs over, the one named last changes fastest.
Arguments:
- tokens: bfloat16 [1024, 3072], P('ep', 'tp'), may hold values from -6 to 6
- routes: int32 [1024, 2], P('ep'), may hold values from 0 to 7, all different within a row; in each aligned block of 128 rows (0 to 127, 128 to 255, ...) at most 40 rows name the same one
- gates: float32 [1024, 2], P('ep'), may hold values from 0.1 to 1.5
- cotangent: bfloat16 [1024, 3072], P('ep', 'tp'), may hold values from -6 to 6
- w_gate: bfloat16 [8, 3072, 896], P('ep', 'tp'), may hold values from -0.109375 to 0.109375
- w_up: bfloat16 [8, 3072, 896], P('ep', 'tp'), may hold values from -0.109375 to 0.109375
- w_down: bfloat16 [8, 3072, 896], P('ep', 'tp'), may hold values from -0.1875 to 0.1875
- shared_hidden: bfloat16 [1024, 448], P('ep'), may hold values from -0.2362278 to 0.2362278
Outputs:
- token_grad: bfloat16 [1024, 3072], P('ep', 'tp')
- gate_grad: float32 [1024, 2], P('ep')
- grad_w_gate: float32 [8, 3072, 896], P('ep', 'tp')
- grad_w_up: float32 [8, 3072, 896], P('ep', 'tp')
- grad_w_down: float32 [8, 3072, 896], P('ep', 'tp')
- row_norms: float32 [3, 8, 3072], P(None, 'ep', 'tp')
- grad_shared: float32 [3072, 448], P('tp', 'ep')
- shared_norms: float32 [3072], P('tp')
The draws below stay inside these ranges and needn't reach their ends.
Inputs may be any that keep to these rules, and one draw needn't show every extreme that they name: `routes`: in each aligned block of 128 rows (the tokens of one index of ep) a row names 2 different experts and no expert is named by more than 40 rows; some expert is named by exactly 40 rows in some blocks.
All inputs are finite; a program needn't handle non-finite values.
Results may differ from the reference program's by a relative error of at most 0.024.
Values may be sent and summed in bfloat16 or wider, within the bound.
A program may use at most 64 MiB of HBM per device.

```python
import math
import jax
import jax.numpy as jnp
import numpy as np
from jax import lax

D = 3072
F = 896
S = 448
TOP_K = 2
TOK_EP = 128
EXPERTS = 8
CAP = 40
TOKENS = 1024
N_EP = 8
N_TP = 4


def draw_shared_hidden(key, part):
    column_key, value_key, row_key = jax.random.split(jax.random.fold_in(key, 17), 3)
    position = jnp.arange(S, dtype=jnp.float32) / S
    columns = jnp.exp(jnp.log(10.0) * position) * jnp.exp(jax.random.uniform(column_key, (S,), jnp.float32, -0.4, 0.4))
    values = jax.random.truncated_normal(value_key, -4.0, 4.0, (TOKENS, S), jnp.float32)
    row_scale = jnp.exp(jax.random.uniform(row_key, (TOKENS, 1), jnp.float32, 0.0, jnp.log(3.0)))
    scale = 1.0 / (3.0 * (TOKENS * S) ** 0.5)
    return (values * columns[None, :] * row_scale * scale).astype(jnp.bfloat16)


def block_levels(key, dims, pieces, least, top_value):
    gain = 1.0
    for dim, blocks in pieces:
        heights = jax.random.uniform(jax.random.fold_in(jax.random.fold_in(key, 6), dim), (blocks,), jnp.float32, least / len(pieces), top_value / len(pieces))
        gain = gain * jnp.repeat(jnp.exp(heights), dims[dim] // blocks).reshape((-1,) + (1,) * (len(dims) - 1 - dim))
    return gain


def deal_out(stream_key, own, number, rows, number_of, top, reach, skew):
    order = jax.random.permutation(stream_key, number_of)
    crowded, common = load_shares(number_of, rows * top, reach, skew, True), load_shares(number_of, rows * top, reach, skew, False)
    places = jnp.arange(number_of)

    def named(tallies, offset_by):
        used = int((tallies > 0).sum())
        fixed = max(1, used // 4)
        moved = fixed + (places - fixed + offset_by * (used - fixed)) % max(1, number_of - fixed)
        return jnp.zeros((number_of,), jnp.int32).at[order[jnp.where(places < fixed, places, moved)]].set(jnp.asarray(tallies, jnp.int32))

    tallies = jnp.where(number % 4 == 0, named(crowded, number // 4), named(common, number - number // 4 - 1))
    mixed = jax.random.permutation(jax.random.fold_in(own, 3), number_of)
    giver, taker = mixed[0:number_of // 2 * 2:2], mixed[1:number_of // 2 * 2:2]
    slack = jnp.minimum(tallies[giver] - 1, reach - tallies[taker]) // 2
    slack = jnp.where((giver == order[0]) | (taker == order[0]) | (tallies[taker] == 0), 0, jnp.maximum(slack, 0))
    moved = jax.random.randint(jax.random.fold_in(own, 4), (number_of // 2,), 0, 1 << 20) % (slack + 1)
    tallies = tallies.at[giver].add(-moved).at[taker].add(moved)
    items = jnp.searchsorted(jnp.cumsum(tallies), jnp.arange(rows * top), side="right").astype(jnp.int32)
    grid = items.reshape(top, rows).T
    grid = grid[jax.random.permutation(jax.random.fold_in(own, 1), rows)]
    offset_by = jax.random.randint(jax.random.fold_in(own, 2), (rows, 1), 0, top)
    return jnp.take_along_axis(grid, (jnp.arange(top)[None, :] + offset_by) % top, axis=1)


def load_shares(number_of, total, reach, skew, full):
    loads = [(1 << 20) // math.isqrt(rank ** skew) + 1 for rank in range(1, number_of + 1)]
    largest = reach if full else min(reach, max(-(-total // number_of), total * loads[0] // sum(loads)))
    least = 1 if total - largest >= number_of - 1 else 0
    given, surplus = [largest] + [least] * (number_of - 1), total - largest - least * (number_of - 1)
    while surplus > 0:
        movable = [i for i in range(1, number_of) if given[i] < largest] or [i for i in range(1, number_of) if given[i] < reach]
        whole, left = sum([loads[i] for i in movable]), surplus
        for i in movable:
            addition = min(reach - given[i], max(1, left * loads[i] // whole), surplus)
            given[i] = given[i] + addition
            surplus = surplus - addition
    return np.array(given)


def normal_values(key, shape, width, most, cuts=(), held_as=jnp.bfloat16):
    result = width * jax.random.normal(key, shape, jnp.float32)
    if cuts:
        result = result * block_levels(key, shape, cuts, -0.22, 0.18)
    return jnp.clip(result, -most, most).astype(held_as)


def setup_inputs(seed: int = 0) -> dict:
    key_list = jax.random.split(jax.random.key(seed), 9)
    tokens = normal_values(key_list[0], (TOKENS, D), 1.0, 6.0, ((0, 8), (1, 4)))
    routes_keys = jax.random.split(jax.random.fold_in(key_list[1], 1), TOKENS // TOK_EP)
    routes_turns = jax.random.permutation(jax.random.fold_in(key_list[1], 3), TOKENS // TOK_EP)
    routes = jax.vmap(lambda own, number: deal_out(jax.random.fold_in(key_list[1], 2), own, number, TOK_EP, EXPERTS, TOP_K, CAP, 2))(routes_keys, routes_turns).reshape((TOKENS, TOP_K))
    gates = jnp.clip(jnp.exp(math.log(1.5) - 2.7080502 * jax.random.uniform(key_list[2], (TOKENS, TOP_K), jnp.float32) ** block_levels(key_list[2], (TOKENS, TOP_K), ((0, 8),), -0.2, 0.2)), 0.1, 1.5)
    cotangent = normal_values(key_list[3], (TOKENS, D), 1.0, 6.0, ((0, 8), (1, 4)))
    w_gate = normal_values(key_list[4], (EXPERTS, D, F), D ** -0.5, 0.109375, ((0, 8), (1, 4)))
    w_up = normal_values(key_list[5], (EXPERTS, D, F), D ** -0.5, 0.109375, ((0, 8), (1, 4)))
    w_down = normal_values(key_list[6], (EXPERTS, D, F), F ** -0.5, 0.1875, ((0, 8), (1, 4)))
    shared_hidden = draw_shared_hidden(jax.random.fold_in(key_list[8], 71), 0)
    return {"tokens": tokens, "routes": routes, "gates": gates, "cotangent": cotangent, "w_gate": w_gate, "w_up": w_up, "w_down": w_down, "shared_hidden": shared_hidden}


def block_targets(block_routes):
    chosen = block_routes.reshape(-1)
    onehot = (chosen[:, None] == jnp.arange(EXPERTS, dtype=jnp.int32)[None, :]).astype(jnp.int32)
    earlier = jnp.cumsum(onehot, axis=0) - onehot
    position = jnp.sum(earlier * onehot, axis=1)
    return (chosen * CAP + position).astype(jnp.int32)


def expert_math(gate_sum, up_sum, down_sum):
    sigma = jax.nn.sigmoid(gate_sum)
    active = gate_sum * sigma
    hidden = (active * up_sum).astype(jnp.bfloat16)
    product = jnp.sum(active * up_sum * down_sum, axis=-1).astype(jnp.bfloat16)
    gate_back = (down_sum * up_sum * sigma * (1.0 + gate_sum * (1.0 - sigma))).astype(jnp.bfloat16)
    up_back = (down_sum * active).astype(jnp.bfloat16)
    return hidden, gate_back, up_back, product


def reference(tokens, routes, gates, cotangent, w_gate, w_up, w_down, shared_hidden):
    pairs = TOK_EP * TOP_K
    rows = N_EP * CAP
    width_part = D // N_TP
    target = jax.vmap(block_targets)(routes.reshape(N_EP, TOK_EP, TOP_K))
    blocks = jnp.arange(N_EP, dtype=jnp.int32)[:, None]
    pair_ids = blocks * pairs + jnp.arange(pairs, dtype=jnp.int32)[None, :]
    source = jnp.zeros((N_EP, EXPERTS * CAP), jnp.int32).at[blocks, target].set(pair_ids)
    filled = jnp.zeros((N_EP, EXPERTS * CAP), jnp.bool_).at[blocks, target].set(True)
    scaled = (gates[:, :, None] * cotangent[:, None, :].astype(jnp.float32)).astype(jnp.bfloat16)
    scaled = scaled.reshape(TOKENS * TOP_K, D)

    def split_sum(left, weight):
        parts = jnp.einsum('rjd,jdf->jrf', left.reshape(rows, N_TP, width_part).astype(jnp.float32),
                           weight.reshape(N_TP, width_part, F).astype(jnp.float32))
        rounded = lax.optimization_barrier(parts.astype(jnp.bfloat16))
        return jnp.sum(rounded.astype(jnp.float32), axis=0)

    def one_expert(expert):
        start = expert * CAP
        picked = lax.dynamic_slice_in_dim(source, start, CAP, 1).reshape(rows)
        live = lax.dynamic_slice_in_dim(filled, start, CAP, 1).reshape(rows)
        token_rows = jnp.where(live[:, None], tokens[picked // TOP_K], jnp.zeros((), jnp.bfloat16))
        grad_rows = jnp.where(live[:, None], scaled[picked], jnp.zeros((), jnp.bfloat16))
        gate_weight = w_gate[expert]
        up_weight = w_up[expert]
        down_weight = w_down[expert]
        gate_sum = split_sum(token_rows, gate_weight)
        up_sum = split_sum(token_rows, up_weight)
        down_sum = split_sum(grad_rows, down_weight)
        hidden, gate_back, up_back, product = expert_math(gate_sum, up_sum, down_sum)
        token_wide = token_rows.astype(jnp.float32)
        grad_gate = jnp.einsum('rd,rf->df', token_wide, gate_back.astype(jnp.float32))
        grad_up = jnp.einsum('rd,rf->df', token_wide, up_back.astype(jnp.float32))
        grad_down = jnp.einsum('rd,rf->df', grad_rows.astype(jnp.float32), hidden.astype(jnp.float32))
        token_back = (jnp.dot(gate_back, gate_weight.T, preferred_element_type=jnp.float32)
                      + jnp.dot(up_back, up_weight.T, preferred_element_type=jnp.float32)).astype(jnp.bfloat16)
        return grad_gate, grad_up, grad_down, token_back, product

    grad_gate, grad_up, grad_down, token_back, product = lax.map(
        one_expert, jnp.arange(EXPERTS, dtype=jnp.int32))
    token_back = token_back.reshape(EXPERTS, N_EP, CAP, D)
    product = product.reshape(EXPERTS, N_EP, CAP)
    expert_of = target // CAP
    slot_of = target % CAP
    per_pair = token_back[expert_of, blocks, slot_of].reshape(TOKENS, TOP_K, D)
    token_grad = jnp.sum(per_pair.astype(jnp.float32), axis=1).astype(jnp.bfloat16)
    gate_grad = product[expert_of, blocks, slot_of].reshape(TOKENS, TOP_K).astype(jnp.float32) / gates
    row_norms = jnp.stack([jnp.sum(grad_gate * grad_gate, axis=-1),
                           jnp.sum(grad_up * grad_up, axis=-1),
                           jnp.sum(grad_down * grad_down, axis=-1)], axis=0)
    grad_shared = jnp.dot(cotangent.T, shared_hidden, preferred_element_type=jnp.float32)
    shared_norms = jnp.sum(grad_shared * grad_shared, axis=1)
    return token_grad, gate_grad, grad_gate, grad_up, grad_down, row_norms, grad_shared, shared_norms
```

```python
import functools

import jax
import jax.numpy as jnp
from jax import lax
from jax.experimental import pallas as pl
from jax.experimental.pallas import tpu as pltpu
from jax.sharding import PartitionSpec as P

MESH = pl.DeviceIdType.MESH
F32 = jnp.float32
BF16 = jnp.bfloat16


def round_up(n, m):
    return -(-n // m) * m


def dot(a, b, ca=1, cb=0):
    return lax.dot_general(a, b, (((ca,), (cb,)), ((), ())), preferred_element_type=F32)


def exchange_kernel(
    n_ep, n_tp, cap,
    tok, cot, rts, gts, gates, sh, wg_h, wu_h, wd_h,
    tg_out, gg_out, gs_out, sn_out, x_out, y_out, act_out,
    hot0, hot1, send_x, send_y, recv_x, recv_y, xs, ys, wg, wu, wd,
    sh_send, sh_recv, nr_send, nr_recv, part, rs_recv, act, prod, back_send, back_recv,
    w_sem, x_ss, x_rs, y_ss, y_rs, s_ss, s_rs, n_ss, n_rs, p_ss, p_rs, a_ss, a_rs,
    q_ss, q_rs, b_ss, b_rs, o_sem,
):
    me = lax.axis_index("ep")
    tp = lax.axis_index("tp")
    width = tok.shape[1]
    count = tok.shape[0]
    hid = wg.shape[1]
    rows = n_ep * cap
    chunk = rows // n_tp
    per_chunk = n_ep // n_tp
    wide = back_send.shape[2] - 128

    weight_copies = [
        pltpu.make_async_copy(h, v, w_sem.at[i])
        for i, (h, v) in enumerate(((wg_h, wg), (wu_h, wu), (wd_h, wd)))
    ]
    for c in weight_copies:
        c.start()

    barrier = pltpu.get_barrier_semaphore()
    for d in range(1, n_ep):
        pl.semaphore_signal(barrier, inc=1, device_id={"ep": lax.rem(me + d, n_ep)}, device_id_type=MESH)
    for d in range(1, n_tp):
        pl.semaphore_signal(barrier, inc=1, device_id={"tp": lax.rem(tp + d, n_tp)}, device_id_type=MESH)

    routes = rts[...]
    experts = lax.broadcasted_iota(jnp.int32, (n_ep, count), 0)
    pick = [(routes[k : k + 1, :] == experts).astype(F32) for k in range(2)]
    before = (
        lax.broadcasted_iota(jnp.int32, (count, count), 0)
        < lax.broadcasted_iota(jnp.int32, (count, count), 1)
    ).astype(BF16)
    earlier = dot((pick[0] + pick[1]).astype(BF16), before)
    row_ids = lax.broadcasted_iota(jnp.int32, (rows, count), 0)
    hits = []
    for k in range(2):
        slot = jnp.sum(pick[k] * earlier, axis=0, keepdims=True).astype(jnp.int32)
        hits.append(row_ids == routes[k : k + 1, :] * cap + slot)
    one = [jnp.where(h, 1.0, 0.0) for h in hits]
    hot0[...] = one[0].astype(BF16)
    hot1[...] = one[1].astype(BF16)
    both = (one[0] + one[1]).astype(BF16)
    gate_col = jnp.sum(
        jnp.where(hits[0], gts[0:1, :], 0.0) + jnp.where(hits[1], gts[1:2, :], 0.0),
        axis=1, keepdims=True,
    )
    send_x[...] = dot(both, tok[...]).reshape(n_ep, cap, width).astype(BF16)

    pl.semaphore_wait(barrier, n_ep - 1 + n_tp - 1)

    def to_ep(src, dst, ss, rs):
        copies = []
        for d in range(1, n_ep):
            peer = lax.rem(me + d, n_ep)
            c = pltpu.make_async_remote_copy(
                src_ref=src(peer), dst_ref=dst(me), send_sem=ss.at[d], recv_sem=rs.at[d],
                device_id={"ep": peer}, device_id_type=MESH,
            )
            c.start()
            copies.append(c)
        return copies

    def to_tp(src, dst, ss, rs):
        copies = []
        for d in range(1, n_tp):
            peer = lax.rem(tp + d, n_tp)
            c = pltpu.make_async_remote_copy(
                src_ref=src(peer), dst_ref=dst(d), send_sem=ss.at[d], recv_sem=rs.at[d],
                device_id={"tp": peer}, device_id_type=MESH,
            )
            c.start()
            copies.append(c)
        return copies

    x_copies = to_ep(lambda p: send_x.at[p], lambda m: recv_x.at[m], x_ss, x_rs)
    send_y[...] = (dot(both, cot[...]) * gate_col).reshape(n_ep, cap, width).astype(BF16)
    y_copies = to_ep(lambda p: send_y.at[p], lambda m: recv_y.at[m], y_ss, y_rs)
    recv_x[me] = send_x[me]
    recv_y[me] = send_y[me]

    depth = sh.shape[0] // n_ep
    sh_send[...] = dot(sh[...], cot[...]).reshape(n_ep, depth, width).astype(BF16)
    s_copies = to_ep(lambda p: sh_send.at[p], lambda m: sh_recv.at[m], s_ss, s_rs)
    sh_recv[me] = sh_send[me]

    for c in weight_copies:
        c.wait()
    for c in x_copies:
        c.wait_recv()
    xs[...] = recv_x[...].astype(F32).reshape(rows, width).astype(BF16)
    p_copies = []

    def partial(i, left, weight):
        part[i] = dot(left[...], weight[...]).astype(BF16).reshape(n_tp, chunk, hid)
        p_copies.append(
            to_tp(lambda p: part.at[i, p], lambda d: rs_recv.at[i, d], p_ss.at[i], p_rs.at[i])
        )

    partial(0, xs, wg)
    partial(1, xs, wu)
    for c in y_copies:
        c.wait_recv()
    ys[...] = recv_y[...].astype(F32).reshape(rows, width).astype(BF16)
    partial(2, ys, wd)
    out_copies = [
        pltpu.make_async_copy(xs, x_out, o_sem.at[0]),
        pltpu.make_async_copy(ys, y_out, o_sem.at[1]),
    ]
    for c in out_copies:
        c.start()

    sums = []
    for i in range(3):
        total = part[i, tp].astype(F32)
        for d in range(1, n_tp):
            p_copies[i][d - 1].wait_recv()
            total = total + rs_recv[i, d].astype(F32)
        sums.append(total)
    gate_sum, up_sum, down_sum = sums
    sigma = jax.nn.sigmoid(gate_sum)
    active = gate_sum * sigma
    act[1, tp] = (down_sum * up_sum * sigma * (1.0 + gate_sum * (1.0 - sigma))).astype(BF16)
    gb_copies = to_tp(lambda p: act.at[1, tp], lambda d: act.at[1, tp], a_ss.at[1], a_rs.at[1])
    act[2, tp] = (down_sum * active).astype(BF16)
    ub_copies = to_tp(lambda p: act.at[2, tp], lambda d: act.at[2, tp], a_ss.at[2], a_rs.at[2])
    hidden = active * up_sum
    product = jnp.sum(hidden * down_sum, axis=1, keepdims=True)
    prod[tp] = jnp.broadcast_to(product, (chunk, 128)).astype(BF16)
    q_copies = to_tp(lambda p: prod.at[tp], lambda d: prod.at[tp], q_ss, q_rs)
    act[0, tp] = hidden.astype(BF16)
    h_copies = to_tp(lambda p: act.at[0, tp], lambda d: act.at[0, tp], a_ss.at[0], a_rs.at[0])

    def back_copy(q, source):
        return pltpu.make_async_remote_copy(
            src_ref=back_send.at[q], dst_ref=back_recv.at[source], send_sem=b_ss.at[q],
            recv_sem=b_rs.at[source], device_id={"ep": q}, device_id_type=MESH,
        )

    def rows_back(j):
        out = dot(act[1, j], wg[...], 1, 1) + dot(act[2, j], wu[...], 1, 1)
        out = out.reshape(per_chunk, cap, width).astype(BF16)
        extra = prod[j].astype(F32).reshape(per_chunk, cap, 128).astype(BF16)
        for i in range(per_chunk):
            q = j * per_chunk + i
            if wide != width:
                back_send[q] = jnp.zeros((cap, wide + 128), BF16)
            back_send[q, :, :width] = out[i]
            back_send[q, :, wide:] = extra[i]

            @pl.when(q != me)
            def _():
                back_copy(q, me).start()

    rows_back(tp)

    for c in s_copies:
        c.wait_recv()
    shared = jnp.sum(sh_recv[...].astype(F32), axis=0)
    gs_out[...] = shared
    nr_send[...] = jnp.broadcast_to(jnp.sum(shared * shared, axis=0, keepdims=True), (8, width))
    n_copies = to_ep(lambda p: nr_send, lambda m: nr_recv.at[m], n_ss, n_rs)
    nr_recv[me] = nr_send[...]

    for d in range(1, n_tp):
        gb_copies[d - 1].wait_recv()
        ub_copies[d - 1].wait_recv()
        q_copies[d - 1].wait_recv()
        rows_back(lax.rem(tp + n_tp - d, n_tp))

    for d in range(1, n_tp):
        h_copies[d - 1].wait_recv()
    act_copy = pltpu.make_async_copy(act, act_out, o_sem.at[2])
    act_copy.start()
    for c in n_copies:
        c.wait_recv()
    sn_out[...] = jnp.sum(nr_recv[...], axis=0)
    back_recv[me] = back_send[me]
    for d in range(1, n_ep):
        source = lax.rem(me + n_ep - d, n_ep)
        back_copy(lax.rem(me + d, n_ep), source).wait_recv()
    back = back_recv[...].astype(F32).reshape(rows, wide + 128).astype(BF16)
    both = (hot0[...].astype(F32) + hot1[...].astype(F32)).astype(BF16)
    tg_out[...] = dot(both, back[:, :width], 0, 0).astype(BF16)
    first = dot(hot0[...], back[:, wide:], 0, 0)[:, :2]
    second = dot(hot1[...], back[:, wide:], 0, 0)[:, :2]
    lane = lax.broadcasted_iota(jnp.int32, (count, 2), 1)
    gg_out[...] = jnp.where(lane == 0, first, second) / gates[...]

    for group in (x_copies, y_copies, s_copies, n_copies, gb_copies, ub_copies, q_copies, h_copies, *p_copies):
        for c in group:
            c.wait_send()
    for d in range(1, n_ep):
        back_copy(lax.rem(me + d, n_ep), me).wait_send()
    for c in (*out_copies, act_copy):
        c.wait()


def grads_kernel(x, y, act, gg, gu, gd, norms):
    for i, (left, which, out) in enumerate(((x, 1, gg), (x, 2, gu), (y, 0, gd))):
        grad = dot(left[...], act[which], 0, 0)
        out[...] = grad
        norms[i, :] = jnp.sum(grad * grad, axis=1)


def on_device(n_ep, n_tp, tokens, routes, gates, cotangent, w_gate, w_up, w_down, shared_hidden):
    count, width = tokens.shape
    top = routes.shape[1]
    hid = w_gate.shape[2]
    cap = round_up(5 * count * top // (4 * n_ep), 8)
    rows = n_ep * cap
    chunk = rows // n_tp
    own = shared_hidden.shape[1] // n_ep
    depth = round_up(own, 16)
    wide = round_up(width, 128)
    sh = shared_hidden.T.reshape(n_ep, own, count)
    sh = jnp.pad(sh, ((0, 0), (0, depth - own), (0, 0))).reshape(n_ep * depth, count)
    vm = pl.BlockSpec(memory_space=pltpu.VMEM)
    hbm = pl.BlockSpec(memory_space=pl.ANY)
    dma = pltpu.SemaphoreType.DMA
    sds = jax.ShapeDtypeStruct
    tg, gg, gs, sn, x, y, act = pl.pallas_call(
        functools.partial(exchange_kernel, n_ep, n_tp, cap),
        out_shape=(
            sds((count, width), BF16), sds((count, top), F32), sds((depth, width), F32),
            sds((8, width), F32), sds((rows, width), BF16), sds((rows, width), BF16),
            sds((3, n_tp, chunk, hid), BF16),
        ),
        in_specs=[vm] * 6 + [hbm] * 3,
        out_specs=(vm, vm, vm, vm, hbm, hbm, hbm),
        scratch_shapes=[
            pltpu.VMEM((rows, count), BF16), pltpu.VMEM((rows, count), BF16),
            *[pltpu.VMEM((n_ep, cap, width), BF16)] * 4,
            *[pltpu.VMEM((rows, width), BF16)] * 2,
            *[pltpu.VMEM((width, hid), BF16)] * 3,
            *[pltpu.VMEM((n_ep, depth, width), BF16)] * 2,
            pltpu.VMEM((8, width), F32), pltpu.VMEM((n_ep, 8, width), F32),
            *[pltpu.VMEM((3, n_tp, chunk, hid), BF16)] * 3,
            pltpu.VMEM((n_tp, chunk, 128), BF16),
            *[pltpu.VMEM((n_ep, cap, wide + 128), BF16)] * 2,
            dma((3,)), *[dma((n_ep,))] * 8, *[dma((3, n_tp))] * 4, *[dma((n_tp,))] * 2,
            *[dma((n_ep,))] * 2, dma((3,)),
        ],
        compiler_params=pltpu.CompilerParams(
            collective_id=0, has_side_effects=True, vmem_limit_bytes=56 * 1024 * 1024
        ),
    )(tokens, cotangent, routes.T, gates.T, gates, sh, w_gate[0], w_up[0], w_down[0])
    act = act.reshape(3, rows, hid)
    tile = 256 if width % 256 == 0 else width
    grad_spec = pl.BlockSpec((tile, hid), lambda i: (i, 0))
    grad_gate, grad_up, grad_down, norms = pl.pallas_call(
        grads_kernel,
        grid=(width // tile,),
        out_shape=(*[sds((width, hid), F32)] * 3, sds((3, width), F32)),
        in_specs=[pl.BlockSpec((rows, tile), lambda i: (0, i))] * 2
        + [pl.BlockSpec((3, rows, hid), lambda i: (0, 0, 0))],
        out_specs=(grad_spec, grad_spec, grad_spec, pl.BlockSpec((3, tile), lambda i: (0, i))),
        compiler_params=pltpu.CompilerParams(vmem_limit_bytes=40 * 1024 * 1024),
    )(x, y, act)
    return (
        tg, gg, grad_gate[None], grad_up[None], grad_down[None], norms[:, None, :],
        gs[:own].T, sn[0],
    )


def solution(mesh):
    return jax.shard_map(
        functools.partial(on_device, mesh.shape["ep"], mesh.shape["tp"]),
        mesh=mesh,
        in_specs=(
            P("ep", "tp"),
            P("ep", None),
            P("ep", None),
            P("ep", "tp"),
            P("ep", "tp", None),
            P("ep", "tp", None),
            P("ep", "tp", None),
            P("ep", None),
        ),
        out_specs=(
            P("ep", "tp"),
            P("ep", None),
            P("ep", "tp", None),
            P("ep", "tp", None),
            P("ep", "tp", None),
            P(None, "ep", "tp"),
            P("tp", "ep"),
            P("tp"),
        ),
        check_vma=False,
    )
```

```python
import functools

import jax
import jax.numpy as jnp
from jax import lax
from jax.experimental import pallas as pl
from jax.experimental.pallas import tpu as pltpu
from jax.sharding import PartitionSpec as P

MESH = pl.DeviceIdType.MESH
F32 = jnp.float32
BF16 = jnp.bfloat16


def round_up(n, m):
    return -(-n // m) * m


def dot(a, b, ca=1, cb=0):
    return lax.dot_general(a, b, (((ca,), (cb,)), ((), ())), preferred_element_type=F32)


def exchange_kernel(
    n_ep, n_tp, cap,
    tok, cot, rts, gts, sh, wg_h, wu_h, wd_h,
    tg_out, gg_out, gs_out, sn_out, x_out, y_out, act_out,
    hot0, hot1, send_x, send_y, recv_x, recv_y, xs, ys, wg, wu, wd,
    sh_send, sh_recv, nr_send, nr_recv, part, rs_recv, act, prod, back_send, back_recv,
    w_sem, x_ss, x_rs, y_ss, y_rs, s_ss, s_rs, n_ss, n_rs, p_ss, p_rs, a_ss, a_rs,
    q_ss, q_rs, b_ss, b_rs, o_sem,
):
    me = lax.axis_index("ep")
    tp = lax.axis_index("tp")
    width = tok.shape[1]
    count = tok.shape[0]
    hid = wg.shape[1]
    rows = n_ep * cap
    chunk = rows // n_tp
    per_chunk = n_ep // n_tp
    wide = back_send.shape[2] - 128

    weight_copies = [
        pltpu.make_async_copy(h, v, w_sem.at[i])
        for i, (h, v) in enumerate(((wg_h, wg), (wu_h, wu), (wd_h, wd)))
    ]
    for c in weight_copies:
        c.start()

    barrier = pltpu.get_barrier_semaphore()
    for d in range(1, n_ep):
        pl.semaphore_signal(barrier, inc=1, device_id={"ep": lax.rem(me + d, n_ep)}, device_id_type=MESH)
    for d in range(1, n_tp):
        pl.semaphore_signal(barrier, inc=1, device_id={"tp": lax.rem(tp + d, n_tp)}, device_id_type=MESH)

    routes = rts[...]
    experts = lax.broadcasted_iota(jnp.int32, (n_ep, count), 0)
    pick = [(routes[k : k + 1, :] == experts).astype(F32) for k in range(2)]
    before = (
        lax.broadcasted_iota(jnp.int32, (count, count), 0)
        < lax.broadcasted_iota(jnp.int32, (count, count), 1)
    ).astype(BF16)
    earlier = dot((pick[0] + pick[1]).astype(BF16), before)
    row_ids = lax.broadcasted_iota(jnp.int32, (rows, count), 0)
    hits = []
    for k in range(2):
        slot = jnp.sum(pick[k] * earlier, axis=0, keepdims=True).astype(jnp.int32)
        hits.append(row_ids == routes[k : k + 1, :] * cap + slot)
    one = [jnp.where(h, 1.0, 0.0) for h in hits]
    hot0[...] = one[0].astype(BF16)
    hot1[...] = one[1].astype(BF16)
    both = (one[0] + one[1]).astype(BF16)
    gate_col = jnp.sum(
        jnp.where(hits[0], gts[0:1, :], 0.0) + jnp.where(hits[1], gts[1:2, :], 0.0),
        axis=1, keepdims=True,
    )
    send_x[...] = dot(both, tok[...]).reshape(n_ep, cap, width).astype(BF16)

    pl.semaphore_wait(barrier, n_ep - 1 + n_tp - 1)

    def to_ep(src, dst, ss, rs):
        copies = []
        for d in range(1, n_ep):
            peer = lax.rem(me + d, n_ep)
            c = pltpu.make_async_remote_copy(
                src_ref=src(peer), dst_ref=dst(me), send_sem=ss.at[d], recv_sem=rs.at[d],
                device_id={"ep": peer}, device_id_type=MESH,
            )
            c.start()
            copies.append(c)
        return copies

    def to_tp(src, dst, ss, rs):
        copies = []
        for d in range(1, n_tp):
            peer = lax.rem(tp + d, n_tp)
            c = pltpu.make_async_remote_copy(
                src_ref=src(peer), dst_ref=dst(d), send_sem=ss.at[d], recv_sem=rs.at[d],
                device_id={"tp": peer}, device_id_type=MESH,
            )
            c.start()
            copies.append(c)
        return copies

    x_copies = to_ep(lambda p: send_x.at[p], lambda m: recv_x.at[m], x_ss, x_rs)
    send_y[...] = (dot(both, cot[...]) * gate_col).reshape(n_ep, cap, width).astype(BF16)
    y_copies = to_ep(lambda p: send_y.at[p], lambda m: recv_y.at[m], y_ss, y_rs)
    recv_x[me] = send_x[me]
    recv_y[me] = send_y[me]

    depth = sh.shape[0] // n_ep
    sh_send[...] = dot(sh[...], cot[...]).reshape(n_ep, depth, width).astype(BF16)
    s_copies = to_ep(lambda p: sh_send.at[p], lambda m: sh_recv.at[m], s_ss, s_rs)
    sh_recv[me] = sh_send[me]

    for c in weight_copies:
        c.wait()
    for c in x_copies:
        c.wait_recv()
    xs[...] = recv_x[...].astype(F32).reshape(rows, width).astype(BF16)
    p_copies = []

    def partial(i, left, weight):
        part[i] = dot(left[...], weight[...]).astype(BF16).reshape(n_tp, chunk, hid)
        p_copies.append(
            to_tp(lambda p: part.at[i, p], lambda d: rs_recv.at[i, d], p_ss.at[i], p_rs.at[i])
        )

    def pair_copy(src, dst, peer, ss, rs):
        c = pltpu.make_async_remote_copy(
            src_ref=src, dst_ref=dst, send_sem=ss, recv_sem=rs,
            device_id={"tp": peer}, device_id_type=MESH,
        )
        c.start()
        return c

    square = n_tp == 4
    x_peer = tp + 1 - 2 * lax.rem(tp, 2)
    y_peer = lax.rem(tp + 2, n_tp)
    across = lax.rem(x_peer + 2, n_tp)
    turns = ((x_peer, y_peer), (y_peer, x_peer))

    def paired(i, left, weight):
        part[i] = dot(left[...], weight[...]).astype(BF16).reshape(n_tp, chunk, hid)
        near = turns[i][0]
        p_copies.append([
            pair_copy(part.at[i, across], rs_recv.at[i, 1], near, p_ss.at[i, 1], p_rs.at[i, 1]),
            pair_copy(part.at[i, near], rs_recv.at[i, 0], near, p_ss.at[i, 0], p_rs.at[i, 0]),
        ])

    def paired_pass(i):
        far = turns[i][1]
        p_copies[i][0].wait_recv()
        rs_recv[i, 3] = (part[i, far].astype(F32) + rs_recv[i, 1].astype(F32)).astype(BF16)
        p_copies[i].append(
            pair_copy(rs_recv.at[i, 3], rs_recv.at[i, 2], far, p_ss.at[i, 2], p_rs.at[i, 2])
        )

    first_step = paired if square else partial
    first_step(0, xs, wg)
    first_step(1, xs, wu)
    for c in y_copies:
        c.wait_recv()
    ys[...] = recv_y[...].astype(F32).reshape(rows, width).astype(BF16)
    partial(2, ys, wd)
    if square:
        paired_pass(0)
        paired_pass(1)
    out_copies = [
        pltpu.make_async_copy(xs, x_out, o_sem.at[0]),
        pltpu.make_async_copy(ys, y_out, o_sem.at[1]),
    ]
    for c in out_copies:
        c.start()

    sums = []
    for i in range(3):
        total = part[i, tp].astype(F32)
        if square and i < 2:
            for c in p_copies[i][1:]:
                c.wait_recv()
            sums.append(total + rs_recv[i, 0].astype(F32) + rs_recv[i, 2].astype(F32))
            continue
        for d in range(1, n_tp):
            p_copies[i][d - 1].wait_recv()
            total = total + rs_recv[i, d].astype(F32)
        sums.append(total)
    gate_sum, up_sum, down_sum = sums
    sigma = jax.nn.sigmoid(gate_sum)
    active = gate_sum * sigma
    act[1, tp] = (down_sum * up_sum * sigma * (1.0 + gate_sum * (1.0 - sigma))).astype(BF16)
    def spread(i):
        if not square:
            return to_tp(lambda p: act.at[i, tp], lambda d: act.at[i, tp], a_ss.at[i], a_rs.at[i])
        return [
            pair_copy(act.at[i, tp], act.at[i, tp], peer, a_ss.at[i, k], a_rs.at[i, k])
            for k, peer in enumerate(turns[i - 1])
        ]

    def relay(i, copies):
        near, far = turns[i - 1]
        copies[0].wait_recv()
        copies.append(
            pair_copy(act.at[i, near], act.at[i, near], far, a_ss.at[i, 2], a_rs.at[i, 2])
        )

    gb_copies = spread(1)
    act[2, tp] = (down_sum * active).astype(BF16)
    ub_copies = spread(2)
    hidden = active * up_sum
    product = jnp.sum(hidden * down_sum, axis=1, keepdims=True)
    prod[tp] = jnp.broadcast_to(product, (chunk, 128)).astype(BF16)
    q_copies = to_tp(lambda p: prod.at[tp], lambda d: prod.at[tp], q_ss, q_rs)
    act[0, tp] = hidden.astype(BF16)
    h_copies = to_tp(lambda p: act.at[0, tp], lambda d: act.at[0, tp], a_ss.at[0], a_rs.at[0])

    def back_copy(q, source):
        return pltpu.make_async_remote_copy(
            src_ref=back_send.at[q], dst_ref=back_recv.at[source], send_sem=b_ss.at[q],
            recv_sem=b_rs.at[source], device_id={"ep": q}, device_id_type=MESH,
        )

    def rows_back(j):
        out = dot(act[1, j], wg[...], 1, 1) + dot(act[2, j], wu[...], 1, 1)
        out = out.reshape(per_chunk, cap, width).astype(BF16)
        extra = prod[j].astype(F32).reshape(per_chunk, cap, 128).astype(BF16)
        for i in range(per_chunk):
            q = j * per_chunk + i
            if wide != width:
                back_send[q] = jnp.zeros((cap, wide + 128), BF16)
            back_send[q, :, :width] = out[i]
            back_send[q, :, wide:] = extra[i]

            @pl.when(q != me)
            def _():
                back_copy(q, me).start()

    rows_back(tp)
    if square:
        relay(1, gb_copies)
        relay(2, ub_copies)

    for c in s_copies:
        c.wait_recv()
    shared = jnp.sum(sh_recv[...].astype(F32), axis=0)
    gs_out[...] = shared[: gs_out.shape[0]]
    nr_send[...] = jnp.broadcast_to(jnp.sum(shared * shared, axis=0, keepdims=True), (8, width))
    n_copies = to_ep(lambda p: nr_send, lambda m: nr_recv.at[m], n_ss, n_rs)
    nr_recv[me] = nr_send[...]

    if square:
        for c in q_copies:
            c.wait_recv()
        ub_copies[1].wait_recv()
        rows_back(x_peer)
        gb_copies[1].wait_recv()
        rows_back(y_peer)
        gb_copies[2].wait_recv()
        ub_copies[2].wait_recv()
        rows_back(across)
    else:
        for d in range(1, n_tp):
            gb_copies[d - 1].wait_recv()
            ub_copies[d - 1].wait_recv()
            q_copies[d - 1].wait_recv()
            rows_back(lax.rem(tp + n_tp - d, n_tp))

    for d in range(1, n_tp):
        h_copies[d - 1].wait_recv()
    act_copy = pltpu.make_async_copy(act, act_out, o_sem.at[2])
    act_copy.start()
    for c in n_copies:
        c.wait_recv()
    sn_out[...] = jnp.sum(nr_recv[...], axis=0)
    back_recv[me] = back_send[me]
    for d in range(1, n_ep):
        source = lax.rem(me + n_ep - d, n_ep)
        back_copy(lax.rem(me + d, n_ep), source).wait_recv()
    back = back_recv[...].astype(F32).reshape(rows, wide + 128).astype(BF16)
    both = (hot0[...].astype(F32) + hot1[...].astype(F32)).astype(BF16)
    tg_out[...] = dot(both, back[:, :width], 0, 0).astype(BF16)
    for k, hot in enumerate((hot0, hot1)):
        gg_out[k : k + 1, :] = dot(back[:, wide:], hot[...], 0, 0)[0:1, :] / gts[k : k + 1, :]

    for group in (x_copies, y_copies, s_copies, n_copies, gb_copies, ub_copies, q_copies, h_copies, *p_copies):
        for c in group:
            c.wait_send()
    for d in range(1, n_ep):
        back_copy(lax.rem(me + d, n_ep), me).wait_send()
    for c in (*out_copies, act_copy):
        c.wait()


def grads_kernel(x, y, act, tg, pg, gs, sn, gg, gu, gd, norms, tg_out, pg_out, gs_out, sn_out):
    @pl.when(pl.program_id(0) == 0)
    def _():
        tg_out[...] = tg[...]
        pg_out[...] = pg[...]
        gs_out[...] = gs[...]
        sn_out[...] = sn[0, :]

    for i, (left, which, out) in enumerate(((x, 1, gg), (x, 2, gu), (y, 0, gd))):
        grad = dot(left[...], act[which], 0, 0)
        out[...] = grad
        norms[i, 0, :] = jnp.sum(grad * grad, axis=1)


def on_device(n_ep, n_tp, tokens, routes, gates, cotangent, w_gate, w_up, w_down, shared_hidden):
    count, width = tokens.shape
    top = routes.shape[1]
    hid = w_gate.shape[2]
    cap = round_up(5 * count * top // (4 * n_ep), 8)
    rows = n_ep * cap
    chunk = rows // n_tp
    own = shared_hidden.shape[1] // n_ep
    depth = round_up(own, 8)
    wide = round_up(width, 128)
    sh = shared_hidden.T.reshape(n_ep, own, count)
    if depth != own:
        sh = jnp.pad(sh, ((0, 0), (0, depth - own), (0, 0)))
    sh = sh.reshape(n_ep * depth, count)
    vm = pl.BlockSpec(memory_space=pltpu.VMEM)
    hbm = pl.BlockSpec(memory_space=pl.ANY)
    dma = pltpu.SemaphoreType.DMA
    sds = jax.ShapeDtypeStruct
    tg, gg, gs, sn, x, y, act = pl.pallas_call(
        functools.partial(exchange_kernel, n_ep, n_tp, cap),
        out_shape=(
            sds((count, width), BF16), sds((top, count), F32), sds((own, width), F32),
            sds((8, width), F32), sds((rows, width), BF16), sds((rows, width), BF16),
            sds((3, n_tp, chunk, hid), BF16),
        ),
        in_specs=[vm] * 5 + [hbm] * 3,
        out_specs=(vm, vm, vm, vm, hbm, hbm, hbm),
        scratch_shapes=[
            pltpu.VMEM((rows, count), BF16), pltpu.VMEM((rows, count), BF16),
            *[pltpu.VMEM((n_ep, cap, width), BF16)] * 4,
            *[pltpu.VMEM((rows, width), BF16)] * 2,
            *[pltpu.VMEM((width, hid), BF16)] * 3,
            *[pltpu.VMEM((n_ep, depth, width), BF16)] * 2,
            pltpu.VMEM((8, width), F32), pltpu.VMEM((n_ep, 8, width), F32),
            *[pltpu.VMEM((3, n_tp, chunk, hid), BF16)] * 3,
            pltpu.VMEM((n_tp, chunk, 128), BF16),
            *[pltpu.VMEM((n_ep, cap, wide + 128), BF16)] * 2,
            dma((3,)), *[dma((n_ep,))] * 8, *[dma((3, max(n_tp, 4)))] * 4, *[dma((n_tp,))] * 2,
            *[dma((n_ep,))] * 2, dma((3,)),
        ],
        compiler_params=pltpu.CompilerParams(
            collective_id=0, has_side_effects=True, vmem_limit_bytes=56 * 1024 * 1024
        ),
    )(tokens, cotangent, routes.T, gates.T, sh, w_gate[0], w_up[0], w_down[0])
    act = act.reshape(3, rows, hid)
    tile = 256 if width % 256 == 0 else width
    grad_spec = pl.BlockSpec((tile, hid), lambda i: (i, 0))
    whole = [pl.BlockSpec(a.shape, lambda i: (0, 0)) for a in (tg, gg, gs, sn)]
    grad_gate, grad_up, grad_down, norms, tg, gg, gs, sn = pl.pallas_call(
        grads_kernel,
        grid=(width // tile,),
        out_shape=(
            *[sds((width, hid), F32)] * 3, sds((3, 1, width), F32), sds(tg.shape, BF16),
            sds(gg.shape, F32), sds(gs.shape, F32), sds((width,), F32),
        ),
        in_specs=[pl.BlockSpec((rows, tile), lambda i: (0, i))] * 2
        + [pl.BlockSpec((3, rows, hid), lambda i: (0, 0, 0))] + whole,
        out_specs=(
            grad_spec, grad_spec, grad_spec, pl.BlockSpec((3, 1, tile), lambda i: (0, 0, i)),
            *whole[:3], pl.BlockSpec((width,), lambda i: (0,)),
        ),
        compiler_params=pltpu.CompilerParams(vmem_limit_bytes=63 * 1024 * 1024),
    )(x, y, act, tg, gg, gs, sn)
    return (
        tg, gg.T, grad_gate[None], grad_up[None], grad_down[None], norms,
        gs.T, sn,
    )


def solution(mesh):
    return jax.shard_map(
        functools.partial(on_device, mesh.shape["ep"], mesh.shape["tp"]),
        mesh=mesh,
        in_specs=(
            P("ep", "tp"),
            P("ep", None),
            P("ep", None),
            P("ep", "tp"),
            P("ep", "tp", None),
            P("ep", "tp", None),
            P("ep", "tp", None),
            P("ep", None),
        ),
        out_specs=(
            P("ep", "tp"),
            P("ep", None),
            P("ep", "tp", None),
            P("ep", "tp", None),
            P("ep", "tp", None),
            P(None, "ep", "tp"),
            P("tp", "ep"),
            P("tp"),
        ),
        check_vma=False,
    )
```

```python
import functools

import jax
import jax.numpy as jnp
from jax import lax
from jax.experimental import pallas as pl
from jax.experimental.pallas import tpu as pltpu
from jax.sharding import PartitionSpec as P

MESH = pl.DeviceIdType.MESH
F32 = jnp.float32
BF16 = jnp.bfloat16


def round_up(n, m):
    return -(-n // m) * m


def dot(a, b, ca=1, cb=0):
    return lax.dot_general(a, b, (((ca,), (cb,)), ((), ())), preferred_element_type=F32)


def exchange_kernel(
    n_ep, n_tp, cap,
    tok, cot, rts, gts, sh, wg_h, wu_h, wd_h,
    tg_out, gg_out, gs_out, sn_out, x_out, y_out, act_out,
    hot0, hot1, send_x, send_y, recv_x, recv_y, xs, ys, wg, wu, wd,
    sh_send, sh_recv, nr_send, nr_recv, part, rs_recv, act, prod, back_send, back_recv,
    w_sem, x_ss, x_rs, y_ss, y_rs, s_ss, s_rs, n_ss, n_rs, p_ss, p_rs, a_ss, a_rs,
    q_ss, q_rs, b_ss, b_rs, o_sem,
):
    me = lax.axis_index("ep")
    tp = lax.axis_index("tp")
    width = tok.shape[1]
    count = tok.shape[0]
    hid = wg.shape[1]
    rows = n_ep * cap
    chunk = rows // n_tp
    per_chunk = n_ep // n_tp
    wide = back_send.shape[2] - 128

    weight_copies = [
        pltpu.make_async_copy(h, v, w_sem.at[i])
        for i, (h, v) in enumerate(((wg_h, wg), (wu_h, wu), (wd_h, wd)))
    ]
    for c in weight_copies:
        c.start()

    barrier = pltpu.get_barrier_semaphore()
    for d in range(1, n_ep):
        pl.semaphore_signal(barrier, inc=1, device_id={"ep": lax.rem(me + d, n_ep)}, device_id_type=MESH)
    for d in range(1, n_tp):
        pl.semaphore_signal(barrier, inc=1, device_id={"tp": lax.rem(tp + d, n_tp)}, device_id_type=MESH)

    routes = rts[...]
    experts = lax.broadcasted_iota(jnp.int32, (n_ep, count), 0)
    pick = [(routes[k : k + 1, :] == experts).astype(F32) for k in range(2)]
    before = (
        lax.broadcasted_iota(jnp.int32, (count, count), 0)
        < lax.broadcasted_iota(jnp.int32, (count, count), 1)
    ).astype(BF16)
    earlier = dot((pick[0] + pick[1]).astype(BF16), before)
    row_ids = lax.broadcasted_iota(jnp.int32, (rows, count), 0)
    hits = []
    for k in range(2):
        slot = jnp.sum(pick[k] * earlier, axis=0, keepdims=True).astype(jnp.int32)
        hits.append(row_ids == routes[k : k + 1, :] * cap + slot)
    one = [jnp.where(h, 1.0, 0.0) for h in hits]
    hot0[...] = one[0].astype(BF16)
    hot1[...] = one[1].astype(BF16)
    both = (one[0] + one[1]).astype(BF16)
    gate_col = jnp.sum(
        jnp.where(hits[0], gts[0:1, :], 0.0) + jnp.where(hits[1], gts[1:2, :], 0.0),
        axis=1, keepdims=True,
    )
    send_x[...] = dot(both, tok[...]).reshape(n_ep, cap, width).astype(BF16)

    pl.semaphore_wait(barrier, n_ep - 1 + n_tp - 1)

    def to_ep(src, dst, ss, rs):
        copies = []
        for d in range(1, n_ep):
            peer = lax.rem(me + d, n_ep)
            c = pltpu.make_async_remote_copy(
                src_ref=src(peer), dst_ref=dst(me), send_sem=ss.at[d], recv_sem=rs.at[d],
                device_id={"ep": peer}, device_id_type=MESH,
            )
            c.start()
            copies.append(c)
        return copies

    def to_tp(src, dst, ss, rs):
        copies = []
        for d in range(1, n_tp):
            peer = lax.rem(tp + d, n_tp)
            c = pltpu.make_async_remote_copy(
                src_ref=src(peer), dst_ref=dst(d), send_sem=ss.at[d], recv_sem=rs.at[d],
                device_id={"tp": peer}, device_id_type=MESH,
            )
            c.start()
            copies.append(c)
        return copies

    x_copies = to_ep(lambda p: send_x.at[p], lambda m: recv_x.at[m], x_ss, x_rs)
    send_y[...] = (dot(both, cot[...]) * gate_col).reshape(n_ep, cap, width).astype(BF16)
    y_copies = to_ep(lambda p: send_y.at[p], lambda m: recv_y.at[m], y_ss, y_rs)
    recv_x[me] = send_x[me]
    recv_y[me] = send_y[me]

    depth = sh.shape[0] // n_ep
    sh_send[...] = dot(sh[...], cot[...]).reshape(n_ep, depth, width).astype(BF16)
    s_copies = to_ep(lambda p: sh_send.at[p], lambda m: sh_recv.at[m], s_ss, s_rs)
    sh_recv[me] = sh_send[me]

    for c in weight_copies:
        c.wait()
    for c in x_copies:
        c.wait_recv()
    xs[...] = recv_x[...].astype(F32).reshape(rows, width).astype(BF16)
    p_copies = []

    def partial(i, left, weight):
        part[i] = dot(left[...], weight[...]).astype(BF16).reshape(n_tp, chunk, hid)
        p_copies.append(
            to_tp(lambda p: part.at[i, p], lambda d: rs_recv.at[i, d], p_ss.at[i], p_rs.at[i])
        )

    def pair_copy(src, dst, peer, ss, rs):
        c = pltpu.make_async_remote_copy(
            src_ref=src, dst_ref=dst, send_sem=ss, recv_sem=rs,
            device_id={"tp": peer}, device_id_type=MESH,
        )
        c.start()
        return c

    square = n_tp == 4
    x_peer = tp + 1 - 2 * lax.rem(tp, 2)
    y_peer = lax.rem(tp + 2, n_tp)
    across = lax.rem(x_peer + 2, n_tp)
    turns = ((x_peer, y_peer), (y_peer, x_peer))

    def paired(i, left, weight):
        part[i] = dot(left[...], weight[...]).astype(BF16).reshape(n_tp, chunk, hid)
        near = turns[i][0]
        p_copies.append([
            pair_copy(part.at[i, across], rs_recv.at[i, 1], near, p_ss.at[i, 1], p_rs.at[i, 1]),
            pair_copy(part.at[i, near], rs_recv.at[i, 0], near, p_ss.at[i, 0], p_rs.at[i, 0]),
        ])

    def paired_pass(i):
        far = turns[i][1]
        p_copies[i][0].wait_recv()
        rs_recv[i, 3] = (part[i, far].astype(F32) + rs_recv[i, 1].astype(F32)).astype(BF16)
        p_copies[i].append(
            pair_copy(rs_recv.at[i, 3], rs_recv.at[i, 2], far, p_ss.at[i, 2], p_rs.at[i, 2])
        )

    first_step = paired if square else partial
    first_step(0, xs, wg)
    first_step(1, xs, wu)
    if square:
        paired_pass(0)
        paired_pass(1)
    for c in y_copies:
        c.wait_recv()
    ys[...] = recv_y[...].astype(F32).reshape(rows, width).astype(BF16)
    partial(2, ys, wd)
    out_copies = [
        pltpu.make_async_copy(xs, x_out, o_sem.at[0]),
        pltpu.make_async_copy(ys, y_out, o_sem.at[1]),
    ]
    for c in out_copies:
        c.start()

    sums = []
    for i in range(3):
        total = part[i, tp].astype(F32)
        if square and i < 2:
            for c in p_copies[i][1:]:
                c.wait_recv()
            sums.append(total + rs_recv[i, 0].astype(F32) + rs_recv[i, 2].astype(F32))
            continue
        for d in range(1, n_tp):
            p_copies[i][d - 1].wait_recv()
            total = total + rs_recv[i, d].astype(F32)
        sums.append(total)
    gate_sum, up_sum, down_sum = sums
    sigma = jax.nn.sigmoid(gate_sum)
    active = gate_sum * sigma
    act[1, tp] = (down_sum * up_sum * sigma * (1.0 + gate_sum * (1.0 - sigma))).astype(BF16)
    def spread(i):
        if not square:
            return to_tp(lambda p: act.at[i, tp], lambda d: act.at[i, tp], a_ss.at[i], a_rs.at[i])
        return [
            pair_copy(act.at[i, tp], act.at[i, tp], peer, a_ss.at[i, k], a_rs.at[i, k])
            for k, peer in enumerate(turns[i - 1])
        ]

    def relay(i, copies):
        near, far = turns[i - 1]
        copies[0].wait_recv()
        copies.append(
            pair_copy(act.at[i, near], act.at[i, near], far, a_ss.at[i, 2], a_rs.at[i, 2])
        )

    gb_copies = spread(1)
    act[2, tp] = (down_sum * active).astype(BF16)
    ub_copies = spread(2)
    hidden = active * up_sum
    product = jnp.sum(hidden * down_sum, axis=1, keepdims=True)
    prod[tp] = jnp.broadcast_to(product, (chunk, 128)).astype(BF16)
    q_copies = to_tp(lambda p: prod.at[tp], lambda d: prod.at[tp], q_ss, q_rs)
    act[0, tp] = hidden.astype(BF16)

    def back_copy(q, source):
        return pltpu.make_async_remote_copy(
            src_ref=back_send.at[q], dst_ref=back_recv.at[source], send_sem=b_ss.at[q],
            recv_sem=b_rs.at[source], device_id={"ep": q}, device_id_type=MESH,
        )

    def rows_back(j):
        out = dot(act[1, j], wg[...], 1, 1) + dot(act[2, j], wu[...], 1, 1)
        out = out.reshape(per_chunk, cap, width).astype(BF16)
        extra = prod[j].astype(F32).reshape(per_chunk, cap, 128).astype(BF16)
        for i in range(per_chunk):
            q = j * per_chunk + i
            if wide != width:
                back_send[q] = jnp.zeros((cap, wide + 128), BF16)
            back_send[q, :, :width] = out[i]
            back_send[q, :, wide:] = extra[i]

            @pl.when(q != me)
            def _():
                back_copy(q, me).start()

    rows_back(tp)
    if square:
        relay(1, gb_copies)
        relay(2, ub_copies)
    h_copies = to_tp(lambda p: act.at[0, tp], lambda d: act.at[0, tp], a_ss.at[0], a_rs.at[0])

    for c in s_copies:
        c.wait_recv()
    shared = jnp.sum(sh_recv[...].astype(F32), axis=0)
    gs_out[...] = shared[: gs_out.shape[0]]
    nr_send[...] = jnp.broadcast_to(jnp.sum(shared * shared, axis=0, keepdims=True), (8, width))
    n_copies = to_ep(lambda p: nr_send, lambda m: nr_recv.at[m], n_ss, n_rs)
    nr_recv[me] = nr_send[...]

    if square:
        for c in q_copies:
            c.wait_recv()
        ub_copies[1].wait_recv()
        rows_back(x_peer)
        gb_copies[1].wait_recv()
        rows_back(y_peer)
        gb_copies[2].wait_recv()
        ub_copies[2].wait_recv()
        rows_back(across)
    else:
        for d in range(1, n_tp):
            gb_copies[d - 1].wait_recv()
            ub_copies[d - 1].wait_recv()
            q_copies[d - 1].wait_recv()
            rows_back(lax.rem(tp + n_tp - d, n_tp))

    for d in range(1, n_tp):
        h_copies[d - 1].wait_recv()
    act_copy = pltpu.make_async_copy(act, act_out, o_sem.at[2])
    act_copy.start()
    for c in n_copies:
        c.wait_recv()
    sn_out[...] = jnp.sum(nr_recv[...], axis=0)
    back_recv[me] = back_send[me]
    for d in range(1, n_ep):
        source = lax.rem(me + n_ep - d, n_ep)
        back_copy(lax.rem(me + d, n_ep), source).wait_recv()
    back = back_recv[...].astype(F32).reshape(rows, wide + 128).astype(BF16)
    both = (hot0[...].astype(F32) + hot1[...].astype(F32)).astype(BF16)
    tg_out[...] = dot(both, back[:, :width], 0, 0).astype(BF16)
    for k, hot in enumerate((hot0, hot1)):
        gg_out[k : k + 1, :] = dot(back[:, wide:], hot[...], 0, 0)[0:1, :] / gts[k : k + 1, :]

    for group in (x_copies, y_copies, s_copies, n_copies, gb_copies, ub_copies, q_copies, h_copies, *p_copies):
        for c in group:
            c.wait_send()
    for d in range(1, n_ep):
        back_copy(lax.rem(me + d, n_ep), me).wait_send()
    for c in (*out_copies, act_copy):
        c.wait()


def grads_kernel(x, y, act, tg, pg, gs, sn, gg, gu, gd, norms, tg_out, pg_out, gs_out, sn_out):
    @pl.when(pl.program_id(0) == 0)
    def _():
        tg_out[...] = tg[...]
        pg_out[...] = pg[...]
        gs_out[...] = gs[...]
        sn_out[...] = sn[0, :]

    for i, (left, which, out) in enumerate(((x, 1, gg), (x, 2, gu), (y, 0, gd))):
        grad = dot(left[...], act[which], 0, 0)
        out[...] = grad
        norms[i, 0, :] = jnp.sum(grad * grad, axis=1)


def on_device(n_ep, n_tp, tokens, routes, gates, cotangent, w_gate, w_up, w_down, shared_hidden):
    count, width = tokens.shape
    top = routes.shape[1]
    hid = w_gate.shape[2]
    cap = round_up(5 * count * top // (4 * n_ep), 8)
    rows = n_ep * cap
    chunk = rows // n_tp
    own = shared_hidden.shape[1] // n_ep
    depth = round_up(own, 8)
    wide = round_up(width, 128)
    sh = shared_hidden.T.reshape(n_ep, own, count)
    if depth != own:
        sh = jnp.pad(sh, ((0, 0), (0, depth - own), (0, 0)))
    sh = sh.reshape(n_ep * depth, count)
    vm = pl.BlockSpec(memory_space=pltpu.VMEM)
    hbm = pl.BlockSpec(memory_space=pl.ANY)
    dma = pltpu.SemaphoreType.DMA
    sds = jax.ShapeDtypeStruct
    tg, gg, gs, sn, x, y, act = pl.pallas_call(
        functools.partial(exchange_kernel, n_ep, n_tp, cap),
        out_shape=(
            sds((count, width), BF16), sds((top, count), F32), sds((own, width), F32),
            sds((8, width), F32), sds((rows, width), BF16), sds((rows, width), BF16),
            sds((3, n_tp, chunk, hid), BF16),
        ),
        in_specs=[vm] * 5 + [hbm] * 3,
        out_specs=(vm, vm, vm, vm, hbm, hbm, hbm),
        scratch_shapes=[
            pltpu.VMEM((rows, count), BF16), pltpu.VMEM((rows, count), BF16),
            *[pltpu.VMEM((n_ep, cap, width), BF16)] * 4,
            *[pltpu.VMEM((rows, width), BF16)] * 2,
            *[pltpu.VMEM((width, hid), BF16)] * 3,
            *[pltpu.VMEM((n_ep, depth, width), BF16)] * 2,
            pltpu.VMEM((8, width), F32), pltpu.VMEM((n_ep, 8, width), F32),
            *[pltpu.VMEM((3, n_tp, chunk, hid), BF16)] * 3,
            pltpu.VMEM((n_tp, chunk, 128), BF16),
            *[pltpu.VMEM((n_ep, cap, wide + 128), BF16)] * 2,
            dma((3,)), *[dma((n_ep,))] * 8, *[dma((3, max(n_tp, 4)))] * 4, *[dma((n_tp,))] * 2,
            *[dma((n_ep,))] * 2, dma((3,)),
        ],
        compiler_params=pltpu.CompilerParams(
            collective_id=0, has_side_effects=True, vmem_limit_bytes=56 * 1024 * 1024
        ),
    )(tokens, cotangent, routes.T, gates.T, sh, w_gate[0], w_up[0], w_down[0])
    act = act.reshape(3, rows, hid)
    tile = 256 if width % 256 == 0 else width
    grad_spec = pl.BlockSpec((tile, hid), lambda i: (i, 0))
    whole = [pl.BlockSpec(a.shape, lambda i: (0, 0)) for a in (tg, gg, gs, sn)]
    grad_gate, grad_up, grad_down, norms, tg, gg, gs, sn = pl.pallas_call(
        grads_kernel,
        grid=(width // tile,),
        out_shape=(
            *[sds((width, hid), F32)] * 3, sds((3, 1, width), F32), sds(tg.shape, BF16),
            sds(gg.shape, F32), sds(gs.shape, F32), sds((width,), F32),
        ),
        in_specs=[pl.BlockSpec((rows, tile), lambda i: (0, i))] * 2
        + [pl.BlockSpec((3, rows, hid), lambda i: (0, 0, 0))] + whole,
        out_specs=(
            grad_spec, grad_spec, grad_spec, pl.BlockSpec((3, 1, tile), lambda i: (0, 0, i)),
            *whole[:3], pl.BlockSpec((width,), lambda i: (0,)),
        ),
        compiler_params=pltpu.CompilerParams(vmem_limit_bytes=63 * 1024 * 1024),
    )(x, y, act, tg, gg, gs, sn)
    return (
        tg, gg.T, grad_gate[None], grad_up[None], grad_down[None], norms,
        gs.T, sn,
    )


def solution(mesh):
    return jax.shard_map(
        functools.partial(on_device, mesh.shape["ep"], mesh.shape["tp"]),
        mesh=mesh,
        in_specs=(
            P("ep", "tp"),
            P("ep", None),
            P("ep", None),
            P("ep", "tp"),
            P("ep", "tp", None),
            P("ep", "tp", None),
            P("ep", "tp", None),
            P("ep", None),
        ),
        out_specs=(
            P("ep", "tp"),
            P("ep", None),
            P("ep", "tp", None),
            P("ep", "tp", None),
            P("ep", "tp", None),
            P(None, "ep", "tp"),
            P("tp", "ep"),
            P("tp"),
        ),
        check_vma=False,
    )
```
